512 devices in a mesh: dp: 4 (over x), kv: 64 (over z, y), tp: 2 (over core).
Axes of the slice: x: 4, y: 4, z: 16, core: 2. Of those that a mesh axis runs over, the one named last changes fastest.
Arguments:
- tokens: bfloat16 [256, 2048], P('dp', 'kv'), may hold values from -6 to 6
- w_qdown: bfloat16 [2048, 768], P('kv'), may hold values from -0.125 to 0.125
- w_kvdown: bfloat16 [2048, 512], P('kv'), may hold values from -0.125 to 0.125
- w_krope: bfloat16 [2048, 32], P('kv'), may hold values from -0.125 to 0.125
- q_gain: bfloat16 [768], replicated, may hold values from 0.099609375 to 1.8984375
- kv_gain: bfloat16 [512], replicated, may hold values from 0.099609375 to 1.8984375
- w_qup: bfloat16 [768, 16, 96], P(None, 'tp'), may hold values from -0.21875 to 0.21875
- w_kup: bfloat16 [512, 16, 64], P(None, 'tp'), may hold values from -0.25 to 0.25
- w_vup: bfloat16 [512, 16, 64], P(None, 'tp'), may hold values from -0.25 to 0.25
- out_gain: bfloat16 [1024], P('tp'), may hold values from 0.099609375 to 1.8984375
- w_out: bfloat16 [1024, 2048], P('tp', 'kv'), may hold values from -0.1875 to 0.1875
- cache_latent: bfloat16 [16, 2048, 512], P('dp', 'kv'), may hold values from -600 to 600
- cache_rope: bfloat16 [16, 2048, 32], P('dp', 'kv'), may hold values from -6 to 6
- lengths: int32 [16], P('dp'), may hold values from 1984 to 2016
- accepted: int32 [16], P('dp'), may hold values from 0 to 16
- parent: int32 [16, 16], P('dp'), may hold values from -1 to 14, as said below
Outputs:
- mixed: bfloat16 [256, 2048], P('dp', 'kv')
- latent_out: bfloat16 [16, 2048, 512], P('dp', 'kv')
- rope_out: bfloat16 [16, 2048, 32], P('dp', 'kv')
The draws below stay inside these ranges and needn't reach their ends.
Inputs may be any that keep to these rules, and one draw needn't show every extreme that they name: parent[s, 0] = -1 and 0 <= parent[s, i] < i for i >= 1.
All inputs are finite; a program needn't handle non-finite values.
Results may differ from the reference program's by a relative error of at most 0.0165.
The reference program's roundings to bfloat16 on the way (of `new_rope`, `q_abs` and `scaled`) count: a program that leaves them out, or rounds other values in their place, can miss the bound.
Values may be sent and summed in bfloat16 or wider, within the bound.
No kernel may reach another device: no remote copies, remote signals or barrier semaphores. Data moves between devices by JAX's collectives and lax.ppermute only.
A program may use at most 64 MiB of HBM per device.

```python
import jax
import jax.numpy as jnp
from jax import lax

D = 2048
QR = 768
KVR = 512
HEADS = 16
NOPE = 64
ROPE = 32
V_DIM = 64
PROPS = 16
POS_DEV = 32
SEQS = 16
TOKENS = 256
CTX = 2048


def draw_cache_latent(key, part):
    normal_part = jnp.clip(jax.random.normal(jax.random.fold_in(key, 11), (SEQS, CTX, KVR), jnp.float32), -6.0, 6.0)
    return normal_part.astype(jnp.bfloat16)


def draw_parent(key, part):
    column = jnp.arange(PROPS, dtype=jnp.int32)
    drawn = jax.random.randint(jax.random.fold_in(key, 21), (SEQS, PROPS), 0, jnp.maximum(column, 1)[None, :])
    return jnp.where(column[None, :] == 0, -1, drawn).astype(jnp.int32)


def set_ends(array, stream_key, low, high):
    extent = array.shape
    index_at = [jax.random.randint(jax.random.fold_in(stream_key, axis), (), 0, extent[axis]) for axis in range(len(extent))]
    array = array.at[tuple(index_at)].set(low)
    longest = extent.index(max(extent))
    index_at[longest] = (index_at[longest] + 1) % extent[longest]
    return array.at[tuple(index_at)].set(high)


def steps_of(key, extent, split, low, high):
    level, own = 1.0, jax.random.fold_in(key, 6)
    for axis_at, shards_of in split:
        heights = jnp.exp(jax.random.uniform(jax.random.fold_in(own, axis_at), (shards_of,), jnp.float32, low / len(split), high / len(split)))
        level = level * jnp.repeat(heights, extent[axis_at] // shards_of).reshape([-1 if axis == axis_at else 1 for axis in range(len(extent))])
    return level


def scatter_about(key, extent, width, reach, cuts=(), kind=jnp.bfloat16):
    values = width * jax.random.normal(key, extent, jnp.float32)
    if cuts:
        values = values * steps_of(key, extent, cuts, -0.22, 0.18)
    return jnp.clip(values, -reach, reach).astype(kind)


def setup_inputs(seed: int = 0) -> dict:
    keys = jax.random.split(jax.random.key(seed), 17)
    return {
        "tokens": scatter_about(keys[0], (TOKENS, D), 1.0, 6.0, ((0, 4), (1, 64))),
        "w_qdown": scatter_about(keys[1], (D, QR), D ** -0.5, 0.125, ((0, 64),)),
        "w_kvdown": scatter_about(keys[2], (D, KVR), D ** -0.5, 0.125, ((0, 64),)),
        "w_krope": scatter_about(keys[3], (D, ROPE), D ** -0.5, 0.125, ((0, 64),)),
        "q_gain": jnp.clip(1.0 + 0.18 * jax.random.normal(keys[4], (QR,), jnp.float32), 0.099609375, 1.8984375).astype(jnp.bfloat16),
        "kv_gain": jnp.clip(1.0 + 0.18 * jax.random.normal(keys[5], (KVR,), jnp.float32), 0.099609375, 1.8984375).astype(jnp.bfloat16),
        "w_qup": scatter_about(keys[6], (QR, HEADS, NOPE + ROPE), QR ** -0.5, 0.21875, ((1, 2),)),
        "w_kup": scatter_about(keys[7], (KVR, HEADS, NOPE), KVR ** -0.5, 0.25, ((1, 2),)),
        "w_vup": scatter_about(keys[8], (KVR, HEADS, V_DIM), KVR ** -0.5, 0.25, ((1, 2),)),
        "out_gain": jnp.clip(1.0 + 0.18 * jax.random.normal(keys[9], (HEADS * V_DIM,), jnp.float32), 0.099609375, 1.8984375).astype(jnp.bfloat16),
        "w_out": scatter_about(keys[10], (HEADS * V_DIM, D), (HEADS * V_DIM) ** -0.5, 0.1875, ((0, 2), (1, 64))),
        "cache_latent": draw_cache_latent(jax.random.fold_in(keys[16], 71), 0),
        "cache_rope": scatter_about(keys[12], (SEQS, CTX, ROPE), 1.0, 6.0, ((0, 4), (1, 64))),
        "lengths": set_ends(jax.random.randint(keys[13], (SEQS,), CTX - POS_DEV - 2 * PROPS, CTX - 2 * PROPS + 1), jax.random.fold_in(keys[13], 1), CTX - POS_DEV - 2 * PROPS, CTX - 2 * PROPS).astype(jnp.int32),
        "accepted": set_ends(jax.random.randint(keys[14], (SEQS,), 0, PROPS + 1), jax.random.fold_in(keys[14], 1), 0, PROPS).astype(jnp.int32),
        "parent": draw_parent(jax.random.fold_in(keys[16], 71), 0),
    }


rope_base = 10000.0
epsilon = 1e-06

def rotate(vector, positions):
    half_size = vector.shape[-1] // 2
    frequency = rope_base ** (-jnp.arange(half_size, dtype=jnp.float32) / half_size)
    angles = positions[..., None] * frequency
    cosine = jnp.cos(angles)
    sine_part = jnp.sin(angles)
    first_half = vector[..., :half_size]
    second_half = vector[..., half_size:]
    return jnp.concatenate([first_half * cosine - second_half * sine_part, second_half * cosine + first_half * sine_part], axis=-1)

def normalize(vector, gain):
    return vector * lax.rsqrt(lax.optimization_barrier(jnp.mean(vector * vector, axis=-1, keepdims=True)) + epsilon) * gain.astype(jnp.float32)

def ancestry(parent):
    proposals = parent.shape[-1]
    column = jnp.arange(proposals, dtype=jnp.int32)
    single = (parent[:, :, None] == column[None, None, :]).astype(jnp.float32)
    reached = jnp.minimum(single + jnp.eye(proposals, dtype=jnp.float32), 1.0)
    for repeat in range(max((proposals - 1).bit_length(), 1)):
        reached = jnp.minimum(jnp.einsum('sij,sjk->sik', reached, reached), 1.0)
    depths = lax.optimization_barrier(jnp.sum(reached, axis=-1)) - 1.0
    return (reached, depths)

def reference(tokens, w_qdown, w_kvdown, w_krope, q_gain, kv_gain, w_qup, w_kup, w_vup, out_gain, w_out, cache_latent, cache_rope, lengths, accepted, parent):
    seq_count, proposals = parent.shape
    q_latent = jnp.dot(tokens, w_qdown, preferred_element_type=jnp.float32)
    kv_latent = jnp.dot(tokens, w_kvdown, preferred_element_type=jnp.float32)
    rope_raw = jnp.dot(tokens, w_krope, preferred_element_type=jnp.float32)
    reached, depths = ancestry(parent)
    valid = (lengths + accepted).astype(jnp.int32)
    positions = (valid[:, None].astype(jnp.float32) + depths).reshape(-1)
    q_normed = normalize(q_latent, q_gain).astype(jnp.bfloat16)
    new_latent = normalize(kv_latent, kv_gain).astype(jnp.bfloat16)
    new_rope = rotate(rope_raw, positions).astype(jnp.bfloat16)
    query = jnp.dot(q_normed, w_qup.reshape(w_qup.shape[0], -1), preferred_element_type=jnp.float32)
    query = query.reshape(-1, HEADS, NOPE + ROPE)
    query_full = jnp.concatenate([query[..., :NOPE], rotate(query[..., NOPE:], positions[:, None])], axis=-1).astype(jnp.bfloat16)
    q_nope = query_full[..., :NOPE]
    q_rotary = query_full[..., NOPE:]
    q_absorbed = jnp.einsum('thn,rhn->thr', q_nope.astype(jnp.float32), w_kup.astype(jnp.float32)).astype(jnp.bfloat16)
    score_scale = (NOPE + ROPE) ** (-0.5)

    def attend(items):
        q_abs, q_rot, latent, rotary, own_latent, own_rotary, limit, allowed = items
        q_abs32 = q_abs.astype(jnp.float32)
        q_rot32 = q_rot.astype(jnp.float32)
        latent32 = latent.astype(jnp.float32)
        own32 = own_latent.astype(jnp.float32)
        cache_scores = (jnp.einsum('phr,kr->phk', q_abs32, latent32) + jnp.einsum('phd,kd->phk', q_rot32, rotary.astype(jnp.float32))) * score_scale
        own_scores = (jnp.einsum('phr,kr->phk', q_abs32, own32) + jnp.einsum('phd,kd->phk', q_rot32, own_rotary.astype(jnp.float32))) * score_scale
        key_pos = jnp.arange(latent.shape[0], dtype=jnp.int32)
        visible = (key_pos < limit)[None, None, :]
        own_visible = (allowed > 0.5)[:, None, :]
        top_value = jnp.maximum(lax.optimization_barrier(jnp.max(jnp.where(visible, cache_scores, -1e+30), axis=-1)), lax.optimization_barrier(jnp.max(jnp.where(own_visible, own_scores, -1e+30), axis=-1)))
        cache_weights = jnp.where(visible, jnp.exp(jnp.where(visible, cache_scores, -1e+30) - top_value[..., None]), 0.0)
        own_weights = jnp.where(own_visible, jnp.exp(jnp.where(own_visible, own_scores, -1e+30) - top_value[..., None]), 0.0)
        summed = lax.optimization_barrier(jnp.sum(cache_weights, axis=-1)) + lax.optimization_barrier(jnp.sum(own_weights, axis=-1))
        cache_round = lax.optimization_barrier(cache_weights.astype(jnp.bfloat16)).astype(jnp.float32)
        own_round = lax.optimization_barrier(own_weights.astype(jnp.bfloat16)).astype(jnp.float32)
        blend = jnp.einsum('phk,kr->phr', cache_round, latent32) + jnp.einsum('phk,kr->phr', own_round, own32)
        return blend / summed[..., None]
    attended = lax.map(attend, (q_absorbed.reshape(seq_count, proposals, HEADS, -1), q_rotary.reshape(seq_count, proposals, HEADS, -1), cache_latent, cache_rope, new_latent.reshape(seq_count, proposals, -1), new_rope.reshape(seq_count, proposals, -1), valid, reached))
    attended = attended.reshape(seq_count * proposals, HEADS, -1)
    head_out = jnp.einsum('thr,rhv->thv', attended, w_vup.astype(jnp.float32), precision=lax.Precision.HIGHEST)
    flat_values = head_out.reshape(seq_count * proposals, -1)
    mean_square = lax.optimization_barrier(jnp.mean(flat_values * flat_values, axis=-1, keepdims=True))
    scaled = (flat_values * out_gain.astype(jnp.float32)).astype(jnp.bfloat16)
    mixed = (jnp.dot(scaled, w_out, preferred_element_type=jnp.float32) * lax.rsqrt(mean_square + epsilon)).astype(jnp.bfloat16)

    def write(cache_rows, new_rows, start):
        return lax.dynamic_update_slice(cache_rows, new_rows, (start.astype(jnp.int32), jnp.int32(0)))
    latent_out = jax.vmap(write)(cache_latent, new_latent.reshape(seq_count, proposals, -1), valid)
    rope_out = jax.vmap(write)(cache_rope, new_rope.reshape(seq_count, proposals, -1), valid)
    return (mixed, latent_out, rope_out)
```

```python
import jax
import jax.numpy as jnp
from jax import lax
from jax.experimental import pallas as pl
from jax.experimental.pallas import tpu as pltpu
from jax.sharding import PartitionSpec as P

HEADS = 16
NOPE = 64
ROPE = 32
V_DIM = 64


FOUR = range(4)
LOWS = ((2, 3, 1, 0), (2, 3, 1, 0), (0, 1, 2, 3), (1, 0, 2, 3))
HIGHS = (2, 3, 0, 1)
YS = (2, 3, 0, 1)


def place_of(high, low, y):
    return (high * 4 + LOWS[high][low]) * 4 + YS[y]


BLOCK = [[place_of(high, low, y) for low in FOUR for y in FOUR] for high in FOUR]
RING = [[place_of(high, low, y) for high in HIGHS for low in FOUR] for y in FOUR]
ROW = [
    [place_of(high, low, y) * 2 + core for y in FOUR for core in (0, 1)]
    for high in FOUR
    for low in FOUR
]


def packed(entries):
    word = sum(entry << 2 * k for k, entry in enumerate(entries))
    return word - (1 << 32) if word >> 31 else word


def entry_of(entries, k):
    return (jnp.int32(packed(entries)) >> (2 * k)) & 3


LOW_AT = [row for lows in LOWS for row in lows]
LOW_OF = [lows.index(row) for lows in LOWS for row in FOUR]
Y_OF = [YS.index(y) for y in FOUR]


rope_base = 10000.0
epsilon = 1e-06
f32 = jnp.float32
bf16 = jnp.bfloat16
i32 = jnp.int32
TINY = -1e30


def iota(shape, dim):
    return lax.broadcasted_iota(i32, shape, dim)


def dot(a, b, precision=None):
    return lax.dot_general(
        a, b, (((1,), (0,)), ((), ())), precision=precision, preferred_element_type=f32
    )


def dot_nt(a, b):
    return lax.dot_general(a, b, (((1,), (1,)), ((), ())), preferred_element_type=f32)


def one_hot(test):
    return jnp.where(test, 1.0, 0.0).astype(bf16)


def rope_spread():
    column = iota((32, 256), 1)
    return one_hot(iota((32, 256), 0) == (column >> 7) * 16 + (column & 15))


def side_by_side(ref):
    rows = ref[...].astype(f32)
    return jnp.concatenate([rows[k : k + 1] for k in range(rows.shape[0])], axis=1)


def started(sources, copies, arrived):
    moves = [pltpu.make_async_copy(a, b, arrived.at[k]) for k, (a, b) in enumerate(zip(sources, copies))]
    for move in moves:
        move.start()
    return moves


def project_body(*refs):
    sources, (out, cosine, sine, reach), copies, arrived = refs[:9], refs[9:13], refs[13:22], refs[22]
    moves = started(sources, copies, arrived)
    for move in moves[:3]:
        move.wait()
    tables_body(*copies[:3], cosine, sine, reach)
    tokens, w_q, w_kv, w_kr, latent, rope = copies[3:]
    row = iota((128, 64), 0)
    token = ((row >> 3) & 3) * 16 + (row >> 5) * 4 + (row & 3)
    pick = one_hot(iota((128, 64), 1) == token)
    spread = rope_spread()
    for move in moves[3:]:
        move.wait()
    rows = dot_nt(pick, tokens[...]).astype(bf16)
    w_kr_spread = dot(w_kr[...], spread).astype(bf16)
    core = lax.axis_index("tp")
    w_core = jnp.where(core == 0, w_q[...], jnp.concatenate([w_kv[...], w_kr_spread], axis=1))
    part = dot(rows, w_core)
    first = ((iota((128, 1), 0) >> 2) & 1) == 0
    part = jnp.where(first, part[:, :384], part[:, 384:])
    part_high = part.astype(bf16)
    part_low = (part - part_high.astype(f32)).astype(bf16)
    out[:, :, 0:384] = part_high.reshape(16, 8, 384)
    out[:, :, 1536:1920] = part_low.reshape(16, 8, 384)
    for s in range(4):
        for g in range(4):
            span = latent[s, 8 * g : 8 * g + 8, :]
            span = jnp.where(core == 0, span[:, :256], span[:, 256:])
            key = rope[s, 8 * g : 8 * g + 8, :]
            for a in range(4):
                out[a * 4 + s, :, 384 + 256 * g : 640 + 256 * g] = span
                out[a * 4 + s, :, 1408 + 32 * g : 1440 + 32 * g] = key


def tables_body(lengths, accepted, parent, cosine, sine, reach):
    s = entry_of(Y_OF, lax.axis_index("kv") & 3)
    valid = lengths[s] + accepted[s]
    line = iota((16, 128), 0)
    masks = jnp.zeros((16, 128), i32)
    seen = []
    for i in range(16):
        mask = jnp.int32(1 << i)
        if i:
            up = parent[s, i]
            for j in range(i):
                mask = mask | jnp.where(up == j, seen[j], 0)
        seen.append(mask)
        masks = jnp.where(line == i, mask, masks)
    lane = iota((16, 128), 1)
    bits = jnp.where(lane < 16, (masks >> jnp.minimum(lane, 15)) & 1, 0).astype(f32)
    depth = jnp.sum(bits, axis=1, keepdims=True) - 1.0
    position = valid.astype(f32) + depth
    shard = lax.axis_index("kv")
    part = entry_of(LOW_OF, shard >> 2)
    row = iota((40, 16), 0)
    token = jnp.where(row < 32, row >> 3, part) * 4 + (row & 3)
    pick = jnp.where(iota((40, 16), 1) == token, 1.0, 0.0)
    spread = dot(pick, jnp.broadcast_to(position, (16, 128)), lax.Precision.HIGHEST)
    k = (iota((40, 128), 1) & 15).astype(f32)
    angle = spread * jnp.exp(k * (-9.210340371976184 / 16.0))
    cosine[...] = jnp.cos(angle)
    sine[...] = jnp.sin(angle)
    row = iota((32, 16), 0)
    pick = one_hot(iota((32, 16), 1) == part * 4 + (row & 3))
    own = jnp.where(shard < 16, dot(pick, bits.astype(bf16)), 0.0)
    lane = iota((32, 128), 1)
    for k in range(4):
        own = jnp.where(lane == 123 + k, (lengths[k] + accepted[k]).astype(f32), own)
    reach[...] = jnp.where(lane == 127, valid.astype(f32), own)


def block_sum_body(parts, out):
    same = one_hot((iota((128, 128), 0) & 7) == (iota((128, 128), 1) & 7))
    total = dot(same, parts[:, :, 0:384].reshape(128, 384))
    total += dot(same, parts[:, :, 1536:1920].reshape(128, 384))
    high = total.astype(bf16)
    low = (total - high.astype(f32)).astype(bf16)
    out[:, :, 0:384] = high.reshape(16, 8, 384)
    out[:, :, 384:768] = low.reshape(16, 8, 384)


def normalize_body(ring, block, cosine, sine, q_gain, kv_gain, w_out, out, key_rope):
    x = jnp.sum(ring[...].astype(f32).reshape(4, 32, 768), axis=0).reshape(4, 8, 768)
    x = x[:, :, 0:384] + x[:, :, 384:768]
    x = jnp.concatenate([x, pltpu.roll(x, 4, 1)], axis=2)
    part = entry_of(LOW_OF, lax.axis_index("kv") >> 2)
    query = x[3]
    for k in range(3):
        query = jnp.where(part == k, x[k], query)
    q_scale = lax.rsqrt(jnp.sum(query * query, axis=1, keepdims=True) * (1.0 / 768) + epsilon)
    q_normed = query * q_scale * side_by_side(q_gain)
    x = x.reshape(32, 768)
    left = x[:, :512]
    kv_scale = lax.rsqrt(jnp.sum(left * left, axis=1, keepdims=True) * (1.0 / 512) + epsilon)
    latents = left * kv_scale * side_by_side(kv_gain)
    cos = cosine[0:32, :]
    sin = sine[0:32, :]
    rope_1 = x[:, 512:640] * cos - x[:, 640:768] * sin
    rope_2 = x[:, 640:768] * cos + x[:, 512:640] * sin
    kv_rows = jnp.concatenate([latents, rope_1, rope_2], axis=1)
    rows = jnp.where(lax.axis_index("tp") == 0, jnp.concatenate([q_normed] * 4, axis=0), kv_rows)
    rows = rows.astype(bf16)
    for g in range(4):
        span = block[:, :, 384 + 256 * g : 640 + 256 * g]
        out[128 * g : 128 * g + 128, :] = span.reshape(128, 256)
    for k in range(3):
        out[512 + 32 * k : 544 + 32 * k, :] = rows[:, 256 * k : 256 * k + 256]
    out[608:640, :] = w_out[:, 0:256]
    out[640:672, :] = w_out[:, 256:512]
    key_rope[...] = block[:, :, 1408:1536].reshape(128, 128)


def attend_body(own, other, far_rope, cosine, sine, reach, w_q, w_k, w_v, *refs):
    caches, (out, fresh), kept, arrived = refs[:2], refs[2:4], refs[4:6], refs[6]
    moves = started(caches, kept, arrived)
    shard = lax.axis_index("kv")
    high = shard >> 4
    part = entry_of(LOW_OF, shard >> 2)
    core = lax.axis_index("tp")
    from_0 = jnp.where(core == 0, own[...], other[...])
    from_1 = jnp.where(core == 0, other[...], own[...])
    spans = [slice(512 + 32 * k, 544 + 32 * k) for k in range(3)]
    q_normed = jnp.concatenate([from_0[span][0:8] for span in spans], axis=1)
    latents = jnp.concatenate([from_1[span] for span in spans[:2]], axis=1)
    rope_1 = from_1[576:608, 0:128]
    rope_2 = from_1[576:608, 128:256]
    cos = cosine[32:40, :]
    sin = sine[32:40, :]
    spans = [(0, 64), (64, 80), (80, 96)]
    w_q = [w_q[96 * h + lo : 96 * h + hi, :] for lo, hi in spans for h in range(8)]
    query = dot_nt(q_normed, jnp.concatenate(w_q, axis=0))
    turned_1 = query[:, 512:640] * cos - query[:, 640:768] * sin
    turned_2 = query[:, 640:768] * cos + query[:, 512:640] * sin
    query = jnp.concatenate([query[:, :512], turned_1, turned_2], axis=1)
    query = jnp.where(iota((8, 1), 0) < 4, query, pltpu.roll(query, 4, 0))
    rows = jnp.broadcast_to(query[None], (4, 8, 768)).reshape(32, 768)
    row = iota((32, 768), 0)
    lane = iota((32, 768), 1)
    head = ((row >> 2) & 1) * 4 + (row >> 3)
    lane_head = jnp.where(lane < 512, lane >> 6, (lane & 127) >> 4)
    rows = jnp.where(head == lane_head, rows, 0.0).astype(bf16)
    q_abs = dot(rows[:, :512], w_k[...]).astype(bf16)
    q_rot = rows[:, 512:]
    row = iota((16, 32), 0)
    pick = one_hot(iota((16, 32), 1) == (row >> 2) * 8 + (row & 3))
    own_latent = dot(pick, latents).astype(bf16)
    own_rope = jnp.concatenate([dot(pick, rope_1), dot(pick, rope_2)], axis=1).astype(bf16)
    fresh[:, 0:512] = own_latent
    fresh[:, 512:640] = jnp.zeros((16, 128), bf16)
    fresh[:, 512:528] = own_rope[:, 0:16]
    fresh[:, 528:544] = own_rope[:, 128:144]
    keys = jnp.concatenate([from_0[0:512], from_1[0:512]], axis=1)
    lane = iota((128, 256), 0)
    column = iota((128, 256), 1)
    entry = (column >> 7) * 16 + (column & 15)
    key_rope = jnp.concatenate(
        [dot(far_rope[...], one_hot(lane == 32 * g + entry)) for g in range(4)], axis=0
    ).astype(bf16)
    scale = (NOPE + ROPE) ** (-0.5)
    score = (dot_nt(q_abs, keys) + dot_nt(q_rot, key_rope)) * scale
    own_score = (dot_nt(q_abs, own_latent) + dot_nt(q_rot, own_rope)) * scale
    key = iota((32, 512), 1)
    source = high * 4 + entry_of(LOW_AT, high * 4 + ((key >> 5) & 3))
    place = (source * 4 + entry_of(YS, (key >> 3) & 3)) * 32 + (key >> 7) * 8 + (key & 7)
    seen = place < reach[:, 127:128].astype(i32)
    own_seen = reach[:, 0:16] > 0.5
    score = jnp.where(seen, score, TINY)
    own_score = jnp.where(own_seen, own_score, TINY)
    top = jnp.maximum(
        jnp.max(score, axis=1, keepdims=True), jnp.max(own_score, axis=1, keepdims=True)
    )
    weight = jnp.where(seen, jnp.exp(score - top), 0.0)
    own_weight = jnp.where(own_seen, jnp.exp(own_score - top), 0.0)
    mass = jnp.sum(weight, axis=1, keepdims=True) + jnp.sum(own_weight, axis=1, keepdims=True)
    blend = dot(weight.astype(bf16), keys) + dot(own_weight.astype(bf16), own_latent)
    blend_high = blend.astype(bf16)
    blend_low = (blend - blend_high.astype(f32)).astype(bf16)
    value = dot_nt(jnp.concatenate([blend_high, blend_low], axis=0), w_v[...])
    value = (value[:32] + value[32:]) / jnp.maximum(mass, 1e-30)
    row = iota((32, 512), 0)
    head = ((row >> 2) & 1) * 4 + (row >> 3)
    value = jnp.where(head == iota((32, 512), 1) >> 6, value, 0.0)
    value = jnp.sum(value.reshape(4, 8, 512), axis=0)
    value = (value + pltpu.roll(value, 4, 0))[0:4].astype(bf16)
    out[:, :, 0:512] = jnp.broadcast_to(value[None], (16, 4, 512))
    mass_log = jnp.where(mass > 0, top + jnp.log(jnp.maximum(mass, 1e-30)), TINY)
    row = iota((32, 128), 0)
    lane = iota((32, 128), 1)
    head = ((row >> 2) & 1) * 4 + (row >> 3)
    mass_log = jnp.where((head == (lane & 7)) & (lane < 24), mass_log, 0.0)
    mass_log = jnp.sum(mass_log.reshape(4, 8, 128), axis=0)
    terms = three_terms(mass_log + pltpu.roll(mass_log, 4, 0))[0:4]
    out[:, :, 512:640] = jnp.broadcast_to(terms[None], (16, 4, 128))
    for move in moves:
        move.wait()


def three_terms(rows):
    high = rows.astype(bf16).astype(f32)
    middle = (rows - high).astype(bf16).astype(f32)
    low = rows - high - middle
    lane = iota(rows.shape, 1)
    terms = jnp.where(lane < 8, high, jnp.where(lane < 16, middle, jnp.where(lane < 24, low, 0.0)))
    return terms.astype(bf16)


def flat_body(parts, fresh, out_gain, out):
    rows = jnp.concatenate([parts[k].astype(f32) for k in range(16)], axis=0)
    lane = iota((128, 512), 0)
    spread = one_hot(((lane & 7) == iota((128, 512), 1) >> 6) & (lane < 24))
    mass_log = dot(rows[:, 512:640].astype(bf16), spread).reshape(4, 16, 512)
    weight = jnp.exp(mass_log - jnp.max(mass_log, axis=0, keepdims=True))
    value = jnp.sum(weight * rows[:, 0:512].reshape(4, 16, 512), axis=0)
    value = value / jnp.sum(weight, axis=0)
    square = jnp.sum(value * value, axis=1, keepdims=True)
    scaled = (value * side_by_side(out_gain)).astype(bf16)
    high = square.astype(bf16).astype(f32)
    middle = (square - high).astype(bf16).astype(f32)
    low = square - high - middle
    lane = iota((16, 128), 1)
    tail = fresh[:, 512:640].astype(f32)
    tail = jnp.where(lane == 32, high, jnp.where(lane == 33, middle, tail))
    tail = jnp.where(lane == 34, low, tail).astype(bf16)
    half = jnp.where(lax.axis_index("tp") == 0, fresh[:, 0:256], fresh[:, 256:512])
    out[:, :, 0:512] = jnp.broadcast_to(scaled[None], (8, 16, 512))
    out[:, :, 512:768] = jnp.broadcast_to(half[None], (8, 16, 256))
    out[:, :, 768:896] = jnp.broadcast_to(tail[None], (8, 16, 128))


def output_body(parts, own, other, reach, latent, rope, *refs):
    (out, *outs), (latent_new, rope_new, arrived) = refs[2:5], refs[5:]
    core = lax.axis_index("tp")
    lane = iota((8, 128), 1)
    terms = one_hot((lane >= 32) & (lane < 35))
    weights = [jnp.concatenate([r[608:640, :], r[640:672, :]], axis=1) for r in (own, other)]
    product = square = 0.0
    for c in range(2):
        chunk = jnp.concatenate([parts[2 * s + c] for s in range(4)], axis=0)
        weight = jnp.where(core == c, weights[0], weights[1])
        product += dot_nt(weight, chunk[:, 0:512])
        square += dot_nt(terms, chunk[:, 768:896])
    scale = lax.rsqrt(square[0:1] * (1.0 / (HEADS * V_DIM)) + epsilon)
    out[...] = (product * scale).astype(bf16)
    shard = lax.axis_index("kv")

    @pl.when(shard >= 62)
    def _():
        place = shard * 32 + iota((32, 16), 0)
        for s in range(4):
            valid = reach[:, 123 + s : 124 + s].astype(i32)
            hit = one_hot(place == valid + iota((32, 16), 1))
            used = jnp.sum(hit.astype(f32), axis=1, keepdims=True) > 0.5
            new = jnp.concatenate([parts[2 * s + c, :, 512:768] for c in range(2)], axis=1)
            latent_new[s] = jnp.where(used, dot(hit, new), latent[s].astype(f32)).astype(bf16)
            placed = dot(hit, parts[2 * s, :, 768:896])[:, 0:32]
            rope_new[s] = jnp.where(used, placed, rope[s].astype(f32)).astype(bf16)
        for move in started((latent_new, rope_new), outs, arrived):
            move.wait()


def kernel_call(body, outs, scalars, name, **options):
    vmem = pl.BlockSpec(memory_space=pltpu.VMEM)
    smem = pl.BlockSpec(memory_space=pltpu.SMEM)

    def call(*args):
        return pl.pallas_call(
            body,
            out_shape=outs,
            in_specs=[smem] * scalars + [vmem] * (len(args) - scalars),
            out_specs=jax.tree.map(lambda _: vmem, outs),
            name=name,
            **options,
            compiler_params=pltpu.CompilerParams(vmem_limit_bytes=24 * 2**20),
        )(*args)

    return call


def shape(dims, kind):
    return jax.ShapeDtypeStruct(dims, kind)


def exchanged(x, groups, axes="kv"):
    return lax.all_to_all(x, axes, 0, 0, axis_index_groups=groups, tiled=True)


def shards(
    tokens,
    w_qdown,
    w_kvdown,
    w_krope,
    q_gain,
    kv_gain,
    w_qup,
    w_kup,
    w_vup,
    out_gain,
    w_out,
    cache_latent,
    cache_rope,
    lengths,
    accepted,
    parent,
):
    w_q = jnp.transpose(w_qup, (1, 2, 0)).reshape(768, 768)
    w_k = jnp.transpose(w_kup, (1, 2, 0)).reshape(512, 512)
    w_v = jnp.transpose(w_vup, (1, 2, 0)).reshape(512, 512)
    gains = [g.reshape(-1, 128) for g in (q_gain, kv_gain, out_gain)]
    vmem = pl.BlockSpec(memory_space=pltpu.VMEM)
    smem = pl.BlockSpec(memory_space=pltpu.SMEM)
    hbm = pl.BlockSpec(memory_space=pltpu.HBM)
    sources = (lengths, accepted, parent, tokens.T, w_qdown, w_kvdown, w_krope, cache_latent, cache_rope)
    sources = [pltpu.with_memory_space_constraint(a, pltpu.HBM) for a in sources]
    table = shape((40, 128), f32)
    block, cosine, sine, reach = pl.pallas_call(
        project_body,
        out_shape=(shape((16, 8, 1920), bf16), table, table, shape((32, 128), f32)),
        in_specs=[hbm] * 9,
        out_specs=(vmem,) * 4,
        scratch_shapes=[pltpu.SMEM(a.shape, a.dtype) for a in sources[:3]]
        + [pltpu.VMEM(a.shape, a.dtype) for a in sources[3:]]
        + [pltpu.SemaphoreType.DMA((9,))],
        name="project",
        compiler_params=pltpu.CompilerParams(vmem_limit_bytes=24 * 2**20),
    )(*sources)
    block = exchanged(block, BLOCK)
    busy = pl.CostEstimate(flops=8_000_000_000, bytes_accessed=2_000_000, transcendentals=0)
    block_sum = kernel_call(
        block_sum_body, shape((16, 8, 768), bf16), 0, "block_sum", cost_estimate=busy
    )
    ring = exchanged(block_sum(block), RING)
    outs = (shape((672, 256), bf16), shape((128, 128), bf16))
    normalize = kernel_call(normalize_body, outs, 0, "normalize")
    own, key_rope = normalize(ring, block, cosine, sine, gains[0], gains[1], w_out.T)
    other = lax.ppermute(own, "tp", [(0, 1), (1, 0)])
    outs = (shape((4, 32, 512), bf16), shape((4, 32, 32), bf16))
    parts, fresh, *kept = pl.pallas_call(
        attend_body,
        out_shape=(shape((16, 4, 640), bf16), shape((16, 640), bf16), *outs),
        in_specs=[vmem] * 11,
        out_specs=(vmem,) * 2 + (hbm,) * 2,
        scratch_shapes=[pltpu.SemaphoreType.DMA((2,))],
        name="attend",
        compiler_params=pltpu.CompilerParams(vmem_limit_bytes=24 * 2**20),
    )(own, other, key_rope, cosine, sine, reach, w_q, w_k, w_v, cache_latent, cache_rope)
    parts = exchanged(parts, RING)
    parts = kernel_call(flat_body, shape((8, 16, 896), bf16), 0, "flat")(parts, fresh, gains[2])
    parts = exchanged(parts, ROW, ("kv", "tp"))
    mixed, latent_out, rope_out = pl.pallas_call(
        output_body,
        out_shape=(shape((32, 64), bf16), *outs),
        in_specs=[vmem] * 6 + [hbm] * 2,
        out_specs=(vmem, hbm, hbm),
        input_output_aliases={6: 1, 7: 2},
        scratch_shapes=[pltpu.VMEM(a.shape, a.dtype) for a in outs]
        + [pltpu.SemaphoreType.DMA((2,))],
        name="output",
        compiler_params=pltpu.CompilerParams(vmem_limit_bytes=24 * 2**20),
    )(parts, own, other, reach, cache_latent, cache_rope, *kept)
    return (mixed.T, latent_out, rope_out)


def solution(mesh):
    in_specs = (
        P("dp", "kv"),
        P("kv", None),
        P("kv", None),
        P("kv", None),
        P(),
        P(),
        P(None, "tp", None),
        P(None, "tp", None),
        P(None, "tp", None),
        P("tp"),
        P("tp", "kv"),
        P("dp", "kv", None),
        P("dp", "kv", None),
        P("dp"),
        P("dp"),
        P("dp", None),
    )
    out_specs = (P("dp", "kv"), P("dp", "kv", None), P("dp", "kv", None))
    return jax.shard_map(
        shards, mesh=mesh, in_specs=in_specs, out_specs=out_specs, check_vma=False
    )
```

```python
import jax
import jax.numpy as jnp
from jax import lax
from jax.experimental import pallas as pl
from jax.experimental.pallas import tpu as pltpu
from jax.sharding import PartitionSpec as P

HEADS = 16
NOPE = 64
ROPE = 32
V_DIM = 64


FOUR = range(4)
LOWS = ((2, 3, 1, 0), (3, 2, 1, 0), (0, 1, 2, 3), (1, 0, 2, 3))
HIGHS = (2, 3, 0, 1)
YS = (2, 3, 0, 1)


def place_of(high, low, y):
    return (high * 4 + LOWS[high][low]) * 4 + YS[y]


BLOCK = [[place_of(high, low, y) for low in FOUR for y in FOUR] for high in FOUR]
RING = [[place_of(high, low, y) for high in HIGHS for low in FOUR] for y in FOUR]
ROW = [
    [place_of(high, low, y) * 2 + core for y in FOUR for core in (0, 1)]
    for high in FOUR
    for low in FOUR
]


def packed(entries):
    word = sum(entry << 2 * k for k, entry in enumerate(entries))
    return word - (1 << 32) if word >> 31 else word


def entry_of(entries, k):
    return (jnp.int32(packed(entries)) >> (2 * k)) & 3


LOW_AT = [row for lows in LOWS for row in lows]
LOW_OF = [lows.index(row) for lows in LOWS for row in FOUR]
Y_OF = [YS.index(y) for y in FOUR]


rope_base = 10000.0
epsilon = 1e-06
f32 = jnp.float32
bf16 = jnp.bfloat16
i32 = jnp.int32
TINY = -1e30


def iota(shape, dim):
    return lax.broadcasted_iota(i32, shape, dim)


def dot(a, b, precision=None):
    return lax.dot_general(
        a, b, (((1,), (0,)), ((), ())), precision=precision, preferred_element_type=f32
    )


def dot_nt(a, b):
    return lax.dot_general(a, b, (((1,), (1,)), ((), ())), preferred_element_type=f32)


def one_hot(test):
    return jnp.where(test, 1.0, 0.0).astype(bf16)


def rope_spread():
    column = iota((32, 256), 1)
    return one_hot(iota((32, 256), 0) == (column >> 7) * 16 + (column & 15))


def side_by_side(ref):
    rows = ref[...].astype(f32)
    return jnp.concatenate([rows[k : k + 1] for k in range(rows.shape[0])], axis=1)


def started(sources, copies, arrived):
    moves = [pltpu.make_async_copy(a, b, arrived.at[k]) for k, (a, b) in enumerate(zip(sources, copies))]
    for move in moves:
        move.start()
    return moves


def project_body(*refs):
    sources, (out, cosine, sine, reach), copies, arrived = refs[:9], refs[9:13], refs[13:22], refs[22]
    moves = started(sources, copies, arrived)
    for move in moves[:3]:
        move.wait()
    tables_body(*copies[:3], cosine, sine, reach)
    tokens, w_q, w_kv, w_kr, latent, rope = copies[3:]
    row = iota((128, 64), 0)
    token = ((row >> 3) & 3) * 16 + (row >> 5) * 4 + (row & 3)
    pick = one_hot(iota((128, 64), 1) == token)
    spread = rope_spread()
    for move in moves[3:]:
        move.wait()
    rows = dot_nt(pick, tokens[...]).astype(bf16)
    w_kr_spread = dot(w_kr[...], spread).astype(bf16)
    core = lax.axis_index("tp")
    w_core = jnp.where(core == 0, w_q[...], jnp.concatenate([w_kv[...], w_kr_spread], axis=1))
    part = dot(rows, w_core)
    first = ((iota((128, 1), 0) >> 2) & 1) == 0
    part = jnp.where(first, part[:, :384], part[:, 384:])
    part_high = part.astype(bf16)
    part_low = (part - part_high.astype(f32)).astype(bf16)
    out[:, :, 0:384] = part_high.reshape(16, 8, 384)
    out[:, :, 1536:1920] = part_low.reshape(16, 8, 384)
    for s in range(4):
        for g in range(4):
            span = latent[s, 8 * g : 8 * g + 8, :]
            span = jnp.where(core == 0, span[:, :256], span[:, 256:])
            key = rope[s, 8 * g : 8 * g + 8, :]
            for a in range(4):
                out[a * 4 + s, :, 384 + 256 * g : 640 + 256 * g] = span
                out[a * 4 + s, :, 1408 + 32 * g : 1440 + 32 * g] = key


def tables_body(lengths, accepted, parent, cosine, sine, reach):
    s = entry_of(Y_OF, lax.axis_index("kv") & 3)
    valid = lengths[s] + accepted[s]
    line = iota((16, 128), 0)
    masks = jnp.zeros((16, 128), i32)
    seen = []
    for i in range(16):
        mask = jnp.int32(1 << i)
        if i:
            up = parent[s, i]
            for j in range(i):
                mask = mask | jnp.where(up == j, seen[j], 0)
        seen.append(mask)
        masks = jnp.where(line == i, mask, masks)
    lane = iota((16, 128), 1)
    bits = jnp.where(lane < 16, (masks >> jnp.minimum(lane, 15)) & 1, 0).astype(f32)
    depth = jnp.sum(bits, axis=1, keepdims=True) - 1.0
    position = valid.astype(f32) + depth
    shard = lax.axis_index("kv")
    part = entry_of(LOW_OF, shard >> 2)
    row = iota((40, 16), 0)
    token = jnp.where(row < 32, row >> 3, part) * 4 + (row & 3)
    pick = jnp.where(iota((40, 16), 1) == token, 1.0, 0.0)
    spread = dot(pick, jnp.broadcast_to(position, (16, 128)), lax.Precision.HIGHEST)
    k = (iota((40, 128), 1) & 15).astype(f32)
    angle = spread * jnp.exp(k * (-9.210340371976184 / 16.0))
    cosine[...] = jnp.cos(angle)
    sine[...] = jnp.sin(angle)
    row = iota((32, 16), 0)
    pick = one_hot(iota((32, 16), 1) == part * 4 + (row & 3))
    own = jnp.where(shard < 16, dot(pick, bits.astype(bf16)), 0.0)
    lane = iota((32, 128), 1)
    for k in range(4):
        own = jnp.where(lane == 123 + k, (lengths[k] + accepted[k]).astype(f32), own)
    reach[...] = jnp.where(lane == 127, valid.astype(f32), own)


def block_sum_body(parts, out):
    same = one_hot((iota((128, 128), 0) & 7) == (iota((128, 128), 1) & 7))
    total = dot(same, parts[:, :, 0:384].reshape(128, 384))
    total += dot(same, parts[:, :, 1536:1920].reshape(128, 384))
    high = total.astype(bf16)
    low = (total - high.astype(f32)).astype(bf16)
    out[:, :, 0:384] = high.reshape(16, 8, 384)
    out[:, :, 384:768] = low.reshape(16, 8, 384)


def normalize_body(ring, block, cosine, sine, q_gain, kv_gain, w_out, out, key_rope):
    x = jnp.sum(ring[...].astype(f32).reshape(4, 32, 768), axis=0).reshape(4, 8, 768)
    x = x[:, :, 0:384] + x[:, :, 384:768]
    x = jnp.concatenate([x, pltpu.roll(x, 4, 1)], axis=2)
    part = entry_of(LOW_OF, lax.axis_index("kv") >> 2)
    query = x[3]
    for k in range(3):
        query = jnp.where(part == k, x[k], query)
    q_scale = lax.rsqrt(jnp.sum(query * query, axis=1, keepdims=True) * (1.0 / 768) + epsilon)
    q_normed = query * q_scale * side_by_side(q_gain)
    x = x.reshape(32, 768)
    left = x[:, :512]
    kv_scale = lax.rsqrt(jnp.sum(left * left, axis=1, keepdims=True) * (1.0 / 512) + epsilon)
    latents = left * kv_scale * side_by_side(kv_gain)
    cos = cosine[0:32, :]
    sin = sine[0:32, :]
    rope_1 = x[:, 512:640] * cos - x[:, 640:768] * sin
    rope_2 = x[:, 640:768] * cos + x[:, 512:640] * sin
    kv_rows = jnp.concatenate([latents, rope_1, rope_2], axis=1)
    rows = jnp.where(lax.axis_index("tp") == 0, jnp.concatenate([q_normed] * 4, axis=0), kv_rows)
    rows = rows.astype(bf16)
    for g in range(4):
        span = block[:, :, 384 + 256 * g : 640 + 256 * g]
        out[128 * g : 128 * g + 128, :] = span.reshape(128, 256)
    for k in range(3):
        out[512 + 32 * k : 544 + 32 * k, :] = rows[:, 256 * k : 256 * k + 256]
    out[608:640, :] = w_out[:, 0:256]
    out[640:672, :] = w_out[:, 256:512]
    key_rope[...] = block[:, :, 1408:1536].reshape(128, 128)


def attend_body(own, other, far_rope, cosine, sine, reach, w_q, w_k, w_v, *refs):
    caches, (out, fresh), kept, arrived = refs[:2], refs[2:4], refs[4:6], refs[6]
    moves = started(caches, kept, arrived)
    shard = lax.axis_index("kv")
    high = shard >> 4
    part = entry_of(LOW_OF, shard >> 2)
    core = lax.axis_index("tp")
    from_0 = jnp.where(core == 0, own[...], other[...])
    from_1 = jnp.where(core == 0, other[...], own[...])
    spans = [slice(512 + 32 * k, 544 + 32 * k) for k in range(3)]
    q_normed = jnp.concatenate([from_0[span][0:8] for span in spans], axis=1)
    latents = jnp.concatenate([from_1[span] for span in spans[:2]], axis=1)
    rope_1 = from_1[576:608, 0:128]
    rope_2 = from_1[576:608, 128:256]
    cos = cosine[32:40, :]
    sin = sine[32:40, :]
    spans = [(0, 64), (64, 80), (80, 96)]
    w_q = [w_q[96 * h + lo : 96 * h + hi, :] for lo, hi in spans for h in range(8)]
    query = dot_nt(q_normed, jnp.concatenate(w_q, axis=0))
    turned_1 = query[:, 512:640] * cos - query[:, 640:768] * sin
    turned_2 = query[:, 640:768] * cos + query[:, 512:640] * sin
    query = jnp.concatenate([query[:, :512], turned_1, turned_2], axis=1)
    query = jnp.where(iota((8, 1), 0) < 4, query, pltpu.roll(query, 4, 0))
    rows = jnp.broadcast_to(query[None], (4, 8, 768)).reshape(32, 768)
    row = iota((32, 768), 0)
    lane = iota((32, 768), 1)
    head = ((row >> 2) & 1) * 4 + (row >> 3)
    lane_head = jnp.where(lane < 512, lane >> 6, (lane & 127) >> 4)
    rows = jnp.where(head == lane_head, rows, 0.0).astype(bf16)
    q_abs = dot(rows[:, :512], w_k[...]).astype(bf16)
    q_rot = rows[:, 512:]
    row = iota((16, 32), 0)
    pick = one_hot(iota((16, 32), 1) == (row >> 2) * 8 + (row & 3))
    own_latent = dot(pick, latents).astype(bf16)
    own_rope = jnp.concatenate([dot(pick, rope_1), dot(pick, rope_2)], axis=1).astype(bf16)
    fresh[:, 0:512] = own_latent
    fresh[:, 512:640] = jnp.zeros((16, 128), bf16)
    fresh[:, 512:528] = own_rope[:, 0:16]
    fresh[:, 528:544] = own_rope[:, 128:144]
    keys = jnp.concatenate([from_0[0:512], from_1[0:512]], axis=1)
    lane = iota((128, 256), 0)
    column = iota((128, 256), 1)
    entry = (column >> 7) * 16 + (column & 15)
    key_rope = jnp.concatenate(
        [dot(far_rope[...], one_hot(lane == 32 * g + entry)) for g in range(4)], axis=0
    ).astype(bf16)
    scale = (NOPE + ROPE) ** (-0.5)
    score = (dot_nt(q_abs, keys) + dot_nt(q_rot, key_rope)) * scale
    own_score = (dot_nt(q_abs, own_latent) + dot_nt(q_rot, own_rope)) * scale
    key = iota((32, 512), 1)
    source = high * 4 + entry_of(LOW_AT, high * 4 + ((key >> 5) & 3))
    place = (source * 4 + entry_of(YS, (key >> 3) & 3)) * 32 + (key >> 7) * 8 + (key & 7)
    seen = place < reach[:, 127:128].astype(i32)
    own_seen = reach[:, 0:16] > 0.5
    score = jnp.where(seen, score, TINY)
    own_score = jnp.where(own_seen, own_score, TINY)
    top = jnp.maximum(
        jnp.max(score, axis=1, keepdims=True), jnp.max(own_score, axis=1, keepdims=True)
    )
    weight = jnp.where(seen, jnp.exp(score - top), 0.0)
    own_weight = jnp.where(own_seen, jnp.exp(own_score - top), 0.0)
    mass = jnp.sum(weight, axis=1, keepdims=True) + jnp.sum(own_weight, axis=1, keepdims=True)
    blend = dot(weight.astype(bf16), keys) + dot(own_weight.astype(bf16), own_latent)
    blend_high = blend.astype(bf16)
    blend_low = (blend - blend_high.astype(f32)).astype(bf16)
    value = dot_nt(jnp.concatenate([blend_high, blend_low], axis=0), w_v[...])
    value = (value[:32] + value[32:]) / jnp.maximum(mass, 1e-30)
    row = iota((32, 512), 0)
    head = ((row >> 2) & 1) * 4 + (row >> 3)
    value = jnp.where(head == iota((32, 512), 1) >> 6, value, 0.0)
    value = jnp.sum(value.reshape(4, 8, 512), axis=0)
    value = (value + pltpu.roll(value, 4, 0))[0:4].astype(bf16)
    out[:, :, 0:512] = jnp.broadcast_to(value[None], (16, 4, 512))
    mass_log = jnp.where(mass > 0, top + jnp.log(jnp.maximum(mass, 1e-30)), TINY)
    row = iota((32, 128), 0)
    lane = iota((32, 128), 1)
    head = ((row >> 2) & 1) * 4 + (row >> 3)
    mass_log = jnp.where((head == (lane & 7)) & (lane < 24), mass_log, 0.0)
    mass_log = jnp.sum(mass_log.reshape(4, 8, 128), axis=0)
    terms = three_terms(mass_log + pltpu.roll(mass_log, 4, 0))[0:4]
    out[:, :, 512:640] = jnp.broadcast_to(terms[None], (16, 4, 128))
    for move in moves:
        move.wait()


def three_terms(rows):
    high = rows.astype(bf16).astype(f32)
    middle = (rows - high).astype(bf16).astype(f32)
    low = rows - high - middle
    lane = iota(rows.shape, 1)
    terms = jnp.where(lane < 8, high, jnp.where(lane < 16, middle, jnp.where(lane < 24, low, 0.0)))
    return terms.astype(bf16)


def flat_body(parts, fresh, out_gain, out):
    rows = jnp.concatenate([parts[k].astype(f32) for k in range(16)], axis=0)
    lane = iota((128, 512), 0)
    spread = one_hot(((lane & 7) == iota((128, 512), 1) >> 6) & (lane < 24))
    mass_log = dot(rows[:, 512:640].astype(bf16), spread).reshape(4, 16, 512)
    weight = jnp.exp(mass_log - jnp.max(mass_log, axis=0, keepdims=True))
    value = jnp.sum(weight * rows[:, 0:512].reshape(4, 16, 512), axis=0)
    value = value / jnp.sum(weight, axis=0)
    square = jnp.sum(value * value, axis=1, keepdims=True)
    scaled = (value * side_by_side(out_gain)).astype(bf16)
    high = square.astype(bf16).astype(f32)
    middle = (square - high).astype(bf16).astype(f32)
    low = square - high - middle
    lane = iota((16, 128), 1)
    tail = fresh[:, 512:640].astype(f32)
    tail = jnp.where(lane == 32, high, jnp.where(lane == 33, middle, tail))
    tail = jnp.where(lane == 34, low, tail).astype(bf16)
    half = jnp.where(lax.axis_index("tp") == 0, fresh[:, 0:256], fresh[:, 256:512])
    out[:, :, 0:512] = jnp.broadcast_to(scaled[None], (8, 16, 512))
    out[:, :, 512:768] = jnp.broadcast_to(half[None], (8, 16, 256))
    out[:, :, 768:896] = jnp.broadcast_to(tail[None], (8, 16, 128))


def output_body(parts, own, other, reach, latent, rope, *refs):
    (out, *outs), (latent_new, rope_new, arrived) = refs[2:5], refs[5:]
    core = lax.axis_index("tp")
    lane = iota((8, 128), 1)
    terms = one_hot((lane >= 32) & (lane < 35))
    weights = [jnp.concatenate([r[608:640, :], r[640:672, :]], axis=1) for r in (own, other)]
    product = square = 0.0
    for c in range(2):
        chunk = jnp.concatenate([parts[2 * s + c] for s in range(4)], axis=0)
        weight = jnp.where(core == c, weights[0], weights[1])
        product += dot_nt(weight, chunk[:, 0:512])
        square += dot_nt(terms, chunk[:, 768:896])
    scale = lax.rsqrt(square[0:1] * (1.0 / (HEADS * V_DIM)) + epsilon)
    out[...] = (product * scale).astype(bf16)
    shard = lax.axis_index("kv")

    @pl.when(shard >= 62)
    def _():
        place = shard * 32 + iota((32, 16), 0)
        for s in range(4):
            valid = reach[:, 123 + s : 124 + s].astype(i32)
            hit = one_hot(place == valid + iota((32, 16), 1))
            used = jnp.sum(hit.astype(f32), axis=1, keepdims=True) > 0.5
            new = jnp.concatenate([parts[2 * s + c, :, 512:768] for c in range(2)], axis=1)
            latent_new[s] = jnp.where(used, dot(hit, new), latent[s].astype(f32)).astype(bf16)
            placed = dot(hit, parts[2 * s, :, 768:896])[:, 0:32]
            rope_new[s] = jnp.where(used, placed, rope[s].astype(f32)).astype(bf16)
        for move in started((latent_new, rope_new), outs, arrived):
            move.wait()


def kernel_call(body, outs, scalars, name, **options):
    vmem = pl.BlockSpec(memory_space=pltpu.VMEM)
    smem = pl.BlockSpec(memory_space=pltpu.SMEM)

    def call(*args):
        return pl.pallas_call(
            body,
            out_shape=outs,
            in_specs=[smem] * scalars + [vmem] * (len(args) - scalars),
            out_specs=jax.tree.map(lambda _: vmem, outs),
            name=name,
            **options,
            compiler_params=pltpu.CompilerParams(vmem_limit_bytes=24 * 2**20),
        )(*args)

    return call


def shape(dims, kind):
    return jax.ShapeDtypeStruct(dims, kind)


def exchanged(x, groups, axes="kv"):
    return lax.all_to_all(x, axes, 0, 0, axis_index_groups=groups, tiled=True)


def shards(
    tokens,
    w_qdown,
    w_kvdown,
    w_krope,
    q_gain,
    kv_gain,
    w_qup,
    w_kup,
    w_vup,
    out_gain,
    w_out,
    cache_latent,
    cache_rope,
    lengths,
    accepted,
    parent,
):
    w_q = jnp.transpose(w_qup, (1, 2, 0)).reshape(768, 768)
    w_k = jnp.transpose(w_kup, (1, 2, 0)).reshape(512, 512)
    w_v = jnp.transpose(w_vup, (1, 2, 0)).reshape(512, 512)
    gains = [g.reshape(-1, 128) for g in (q_gain, kv_gain, out_gain)]
    vmem = pl.BlockSpec(memory_space=pltpu.VMEM)
    smem = pl.BlockSpec(memory_space=pltpu.SMEM)
    hbm = pl.BlockSpec(memory_space=pltpu.HBM)
    sources = (lengths, accepted, parent, tokens.T, w_qdown, w_kvdown, w_krope, cache_latent, cache_rope)
    sources = [pltpu.with_memory_space_constraint(a, pltpu.HBM) for a in sources]
    table = shape((40, 128), f32)
    block, cosine, sine, reach = pl.pallas_call(
        project_body,
        out_shape=(shape((16, 8, 1920), bf16), table, table, shape((32, 128), f32)),
        in_specs=[hbm] * 9,
        out_specs=(vmem,) * 4,
        scratch_shapes=[pltpu.SMEM(a.shape, a.dtype) for a in sources[:3]]
        + [pltpu.VMEM(a.shape, a.dtype) for a in sources[3:]]
        + [pltpu.SemaphoreType.DMA((9,))],
        name="project",
        compiler_params=pltpu.CompilerParams(vmem_limit_bytes=24 * 2**20),
    )(*sources)
    block = exchanged(block, BLOCK)
    busy = pl.CostEstimate(flops=8_000_000_000, bytes_accessed=2_000_000, transcendentals=0)
    block_sum = kernel_call(
        block_sum_body, shape((16, 8, 768), bf16), 0, "block_sum", cost_estimate=busy
    )
    ring = exchanged(block_sum(block), RING)
    outs = (shape((672, 256), bf16), shape((128, 128), bf16))
    normalize = kernel_call(normalize_body, outs, 0, "normalize")
    own, key_rope = normalize(ring, block, cosine, sine, gains[0], gains[1], w_out.T)
    other = lax.ppermute(own, "tp", [(0, 1), (1, 0)])
    outs = (shape((4, 32, 512), bf16), shape((4, 32, 32), bf16))
    parts, fresh, *kept = pl.pallas_call(
        attend_body,
        out_shape=(shape((16, 4, 640), bf16), shape((16, 640), bf16), *outs),
        in_specs=[vmem] * 11,
        out_specs=(vmem,) * 2 + (hbm,) * 2,
        scratch_shapes=[pltpu.SemaphoreType.DMA((2,))],
        name="attend",
        compiler_params=pltpu.CompilerParams(vmem_limit_bytes=24 * 2**20),
    )(own, other, key_rope, cosine, sine, reach, w_q, w_k, w_v, cache_latent, cache_rope)
    parts = exchanged(parts, RING)
    parts = kernel_call(flat_body, shape((8, 16, 896), bf16), 0, "flat")(parts, fresh, gains[2])
    parts = exchanged(parts, ROW, ("kv", "tp"))
    mixed, latent_out, rope_out = pl.pallas_call(
        output_body,
        out_shape=(shape((32, 64), bf16), *outs),
        in_specs=[vmem] * 6 + [hbm] * 2,
        out_specs=(vmem, hbm, hbm),
        input_output_aliases={6: 1, 7: 2},
        scratch_shapes=[pltpu.VMEM(a.shape, a.dtype) for a in outs]
        + [pltpu.SemaphoreType.DMA((2,))],
        name="output",
        compiler_params=pltpu.CompilerParams(vmem_limit_bytes=24 * 2**20),
    )(parts, own, other, reach, cache_latent, cache_rope, *kept)
    return (mixed.T, latent_out, rope_out)


def solution(mesh):
    in_specs = (
        P("dp", "kv"),
        P("kv", None),
        P("kv", None),
        P("kv", None),
        P(),
        P(),
        P(None, "tp", None),
        P(None, "tp", None),
        P(None, "tp", None),
        P("tp"),
        P("tp", "kv"),
        P("dp", "kv", None),
        P("dp", "kv", None),
        P("dp"),
        P("dp"),
        P("dp", None),
    )
    out_specs = (P("dp", "kv"), P("dp", "kv", None), P("dp", "kv", None))
    return jax.shard_map(
        shards, mesh=mesh, in_specs=in_specs, out_specs=out_specs, check_vma=False
    )
```
